256 devices in a mesh: ep: 32 (over z, x), tp: 8 (over y, core).
Axes of the slice: x: 4, y: 4, z: 8, core: 2. Of those that a mesh axis runs over, the one named last changes fastest.
Arguments:
- stream: bfloat16 [8192, 3072], P('ep'), may hold values from -30 to 30
- ffn_gain: bfloat16 [3072], replicated, may hold values from 0.099609375 to 1.8984375
- chosen: int32 [32, 1024], replicated, may hold values from 0 to 8191, as said below
- affinity: float32 [32, 1024], P('ep'), may hold values from 0.5 to 2
- w_gate: bfloat16 [32, 3072, 3072], P('ep', None, 'tp'), may hold values from -0.109375 to 0.109375
- w_up: bfloat16 [32, 3072, 3072], P('ep', None, 'tp'), may hold values from -0.109375 to 0.109375
- w_down: bfloat16 [32, 3072, 3072], P('ep', 'tp'), may hold values from -0.109375 to 0.109375
- final_gain: bfloat16 [3072], P('tp'), may hold values from 0.099609375 to 1.8984375
Outputs:
- normed: bfloat16 [8192, 3072], P('ep', 'tp')
The draws below stay inside these ranges and needn't reach their ends.
Inputs may be any that keep to these rules, and one draw needn't show every extreme that they name: `chosen`: row e holds 1024 distinct token numbers in ascending order. Of the 256 tokens of one index of ep, each expert reads at least one and at most 48; in every draw some expert reads exactly 48 from some index.
All inputs are finite; a program needn't handle non-finite values.
Results may differ from the reference program's by a relative error of at most 0.015.
Values may be sent and summed in bfloat16 or wider, within the bound.
A program may use at most 128 MiB of HBM per device.

```python
import math
import jax
import jax.numpy as jnp
from jax import lax

D = 3072
FF = 3072
TOK_DEV = 256
TOKENS = 8192
EXPERTS = 32
CAP = 1024
N_EP = 32
N_TP = 8


def draw_stream(key, part):
    key_base, key_rows, key_cols = jax.random.split(key, 3)
    ramp = jnp.arange(D, dtype=jnp.float32) / D
    columns = jnp.exp(math.log(0.6) + ramp * math.log(3.0)) * jnp.exp(jax.random.uniform(key_cols, (D,), jnp.float32, -0.3, 0.3))
    base = jnp.clip(jax.random.normal(key_base, (TOKENS, D), jnp.float32), -4.0, 4.0)
    rows_scale = jnp.exp(jax.random.uniform(key_rows, (TOKENS, 1), jnp.float32, math.log(0.3), math.log(3.0)))
    return (base * rows_scale * columns[None, :]).astype(jnp.bfloat16)


def draw_chosen(key, part):
    mean_count = TOK_DEV // 8
    spread = TOK_DEV // 16
    pairs = N_EP // 2
    key_diff, key_pick, key_sign, key_score = jax.random.split(key, 4)
    diff = jax.random.randint(key_diff, (EXPERTS, pairs), -spread, spread + 1)
    forced = jax.random.randint(key_pick, (EXPERTS,), 0, pairs)
    signs = jax.random.randint(key_sign, (EXPERTS,), 0, 2) * 2 - 1
    diff = jnp.where(jnp.arange(pairs)[None, :] == forced[:, None], signs[:, None] * spread, diff)
    counts = jnp.stack([mean_count + diff, mean_count - diff], axis=2).reshape(EXPERTS, N_EP)
    scores = jax.random.randint(key_score, (EXPERTS, N_EP, TOK_DEV), 0, 65536) * TOK_DEV + jnp.arange(TOK_DEV)[None, None, :]
    ranks = jnp.argsort(jnp.argsort(scores, axis=-1), axis=-1)
    selected = (ranks < counts[:, :, None]).reshape(EXPERTS, TOKENS)
    positions = jnp.arange(TOKENS, dtype=jnp.int32)[None, :]
    keyed = jnp.where(selected, positions, positions + TOKENS)
    return jnp.sort(keyed, axis=-1)[:, :CAP].astype(jnp.int32)


def block_scale(own_key, shape, cuts, smallest, high):
    gain = 1.0
    for position, shards_of in cuts:
        steps = jax.random.uniform(jax.random.fold_in(jax.random.fold_in(own_key, 6), position), (shards_of,), jnp.float32, smallest / len(cuts), high / len(cuts))
        gain = gain * jnp.repeat(jnp.exp(steps), shape[position] // shards_of).reshape((-1,) + (1,) * (len(shape) - 1 - position))
    return gain


def centred(own_key, dims, scale, bound, shards=(), kind=jnp.bfloat16):
    values = jax.random.normal(own_key, dims, jnp.float32) * scale
    if len(shards) > 0:
        values = block_scale(own_key, dims, shards, -0.22, 0.18) * values
    return jnp.clip(values, min=-bound, max=bound).astype(kind)


def setup_inputs(seed: int = 0) -> dict:
    key_of = jax.random.split(jax.random.key(seed), 9)
    stream = draw_stream(jax.random.fold_in(key_of[8], 71), 0)
    ffn_gain = jnp.clip(1.0 + 0.18 * jax.random.normal(key_of[1], (D,), jnp.float32), 0.099609375, 1.8984375).astype(jnp.bfloat16)
    chosen = draw_chosen(jax.random.fold_in(key_of[8], 71), 0)
    affinity = jnp.clip(jnp.exp(math.log(2.0) - 1.3862944 * jax.random.uniform(key_of[3], (EXPERTS, CAP), jnp.float32) ** block_scale(key_of[3], (EXPERTS, CAP), ((0, 32),), -0.2, 0.2)), 0.5, 2.0)
    w_gate = centred(key_of[4], (EXPERTS, D, FF), D ** -0.5, 0.109375, ((0, 32), (2, 8)))
    w_up = centred(key_of[5], (EXPERTS, D, FF), D ** -0.5, 0.109375, ((0, 32), (2, 8)))
    w_down = centred(key_of[6], (EXPERTS, FF, D), FF ** -0.5, 0.109375, ((0, 32), (1, 8)))
    final_gain = jnp.clip(1.0 + 0.18 * jax.random.normal(key_of[7], (D,), jnp.float32), 0.099609375, 1.8984375).astype(jnp.bfloat16)
    return dict(stream=stream, ffn_gain=ffn_gain, chosen=chosen, affinity=affinity, w_gate=w_gate, w_up=w_up, w_down=w_down, final_gain=final_gain)


EPSILON = 1e-06

def reference(stream, ffn_gain, chosen, affinity, w_gate, w_up, w_down, final_gain):
    widened = stream.astype(jnp.float32)
    scale_in = lax.rsqrt(lax.optimization_barrier(jnp.mean(widened * widened, axis=-1, keepdims=True)) + EPSILON)
    normed_in = (widened * scale_in * ffn_gain.astype(jnp.float32)).astype(jnp.bfloat16)
    block = FF // N_TP

    def one_expert(update, items):
        token_ids, weights, gate_rows, up_rows, down_rows = items
        picked = normed_in[token_ids]
        gate = jnp.dot(picked, gate_rows, preferred_element_type=jnp.float32)
        up = jnp.dot(picked, up_rows, preferred_element_type=jnp.float32)
        hidden = (jax.nn.silu(gate) * up).astype(jnp.bfloat16)
        blocks = hidden.reshape(CAP, N_TP, block).astype(jnp.float32)
        down_blocks = down_rows.reshape(N_TP, block, D).astype(jnp.float32)
        partial_value = jnp.einsum('cjf,jfd->jcd', blocks, down_blocks).astype(jnp.bfloat16)
        summed = lax.optimization_barrier(jnp.sum(partial_value.astype(jnp.float32), axis=0))
        result = (summed * weights[:, None]).astype(jnp.bfloat16)
        return (update.at[token_ids].add(result.astype(jnp.float32)), None)
    update, unused = lax.scan(one_expert, jnp.zeros((TOKENS, D), jnp.float32), (chosen, affinity, w_gate, w_up, w_down))
    merged = widened + update
    scale_out = lax.rsqrt(lax.optimization_barrier(jnp.mean(merged * merged, axis=-1, keepdims=True)) + EPSILON)
    return (merged * scale_out * final_gain.astype(jnp.float32)).astype(jnp.bfloat16)
```

```python
import jax
import jax.numpy as jnp
from jax import lax
from jax.experimental import pallas as pl
from jax.experimental.pallas import tpu as pltpu
from jax.sharding import PartitionSpec as P

EPSILON = 1e-06
MESH = pl.DeviceIdType.MESH
F32, BF16 = jnp.float32, jnp.bfloat16

NZ, NX, NY = 8, 4, 4
EP, TP = NZ * NX, NY * 2
TOK, WIDTH, PICKS = 256, 3072, 1024
SHARE = WIDTH // TP
SLOTS = 48
ROWS = EP * SLOTS
LANE = 128
CHUNKS = SHARE // LANE
HALF = PICKS // 2
STEP = 256


def dot(a, b):
    return jnp.dot(a, b, preferred_element_type=F32)


def columns_of(row):
    return jnp.broadcast_to(row, (LANE, LANE)).T


def kernel(
    stream, gain_in, gain_out, local_row, arrival_row, affinity_row, gate_hbm, up_hbm, down_hbm,
    out,
    gate_w, up_w, down_w, scaled, place, place_t, pick, pick_t, weight_col,
    sending, arrived, picked, gate_acc, up_acc, hidden,
    own_acc, twin_out, twin_in, sums, ring_l, ring_r, fin_l, fin_r, weighted,
    leaving, returned, merged, totals,
    load_sem, out_send, out_recv, ag_send, ag_recv, rs_send, rs_recv, back_send, back_recv,
    tot_send, tot_recv,
):
    me = lax.axis_index("ep")
    tp = lax.axis_index("tp")
    z, x = me // NX, me % NX
    y, core = tp // 2, tp % 2
    y_r, y_l, y_f = (y + 1) % NY, (y + NY - 1) % NY, (y + 2) % NY
    right = (me, y_r * 2 + core)
    left = (me, y_l * 2 + core)
    twin = (me, y * 2 + 1 - core)

    def peer(j):
        jz, jx = j % NZ, j // NZ
        odd = jz % 2
        dz = odd * ((jz + 1) // 2) + (1 - odd) * ((NZ - jz // 2) % NZ)
        return ((z + dz) % NZ) * NX + (x + jx) % NX

    loads = [
        pltpu.make_async_copy(src, dst, load_sem.at[i])
        for i, (src, dst) in enumerate(((gate_hbm, gate_w), (up_hbm, up_w), (down_hbm, down_w)))
    ]
    for load in loads:
        load.start()

    barrier = pltpu.get_barrier_semaphore()

    @pl.loop(1, EP)
    def _(j):
        pl.semaphore_signal(barrier, inc=1, device_id=(peer(j), tp), device_id_type=MESH)

    @pl.loop(1, TP)
    def _(j):
        pl.semaphore_signal(barrier, inc=1, device_id=(me, (tp + j) % TP), device_id_type=MESH)

    own_lanes = pl.ds(pl.multiple_of(tp * SHARE, LANE), SHARE)

    @pl.loop(0, TOK // 32)
    def _(i):
        rows = pl.ds(pl.multiple_of(i * 32, 32), 32)
        wide = stream[rows, :].astype(F32)
        scale = lax.rsqrt(jnp.sum(wide * wide, axis=1, keepdims=True) / WIDTH + EPSILON)
        own = stream[rows, own_lanes].astype(F32)
        scaled[rows, :] = (own * scale * gain_in[:, own_lanes].astype(F32)).astype(BF16)

    @pl.loop(0, ROWS // LANE)
    def _(i):
        rows = pl.ds(pl.multiple_of(i * LANE, LANE), LANE)
        column = columns_of(local_row[:, rows])
        for b in range(TOK // LANE):
            lanes = lax.broadcasted_iota(jnp.int32, (LANE, LANE), 1) + b * LANE
            place[rows, b * LANE:(b + 1) * LANE] = jnp.where(column == lanes, 1.0, 0.0).astype(BF16)

    @pl.loop(0, EP // 8)
    def _(i):
        rows = pl.ds(pl.multiple_of(i * 8 * SLOTS, LANE), 8 * SLOTS)
        taken = dot(place[rows, :], scaled[...]).astype(BF16)
        for k in range(CHUNKS):
            sending[k, pl.ds(i * 8, 8)] = taken[:, k * LANE:(k + 1) * LANE].reshape(8, SLOTS, LANE)

    pl.semaphore_wait(barrier, EP - 1 + TP - 1)

    def exchange(source, target, send, recv, k):
        @pl.loop(1, EP)
        def _(j):
            other = peer(j)
            pltpu.make_async_remote_copy(
                src_ref=source.at[k, other], dst_ref=target.at[k, me],
                send_sem=send.at[k], recv_sem=recv.at[k],
                device_id=(other, tp), device_id_type=MESH,
            ).start()

    def exchange_wait(target, sem, k):
        whole = target.at[k, pl.ds(0, EP - 1)]
        pltpu.make_async_copy(whole, whole, sem.at[k]).wait()

    for k in range(CHUNKS):
        exchange(sending, arrived, out_send, out_recv, k)
    for k in range(CHUNKS):
        arrived[k, me] = sending[k, me]

    @pl.loop(0, PICKS // LANE)
    def _(i):
        rows = pl.ds(pl.multiple_of(i * LANE, LANE), LANE)
        column = columns_of(arrival_row[:, rows])
        for b in range(ROWS // LANE):
            lanes = lax.broadcasted_iota(jnp.int32, (LANE, LANE), 1) + b * LANE
            pick[rows, b * LANE:(b + 1) * LANE] = jnp.where(column == lanes, 1.0, 0.0).astype(BF16)
        weight_col[rows, :] = columns_of(affinity_row[:, rows])

    @pl.loop(0, ROWS // LANE)
    def _(i):
        rows = pl.ds(pl.multiple_of(i * LANE, LANE), LANE)
        subl = lax.broadcasted_iota(jnp.int32, (LANE, PICKS), 0) + i * LANE
        pick_t[rows, :] = jnp.where(arrival_row[...] == subl, 1.0, 0.0).astype(BF16)

    for b in range(TOK // LANE):
        rows = slice(b * LANE, (b + 1) * LANE)
        subl = lax.broadcasted_iota(jnp.int32, (LANE, ROWS), 0) + b * LANE
        place_t[rows, :] = jnp.where(local_row[...] == subl, 1.0, 0.0).astype(BF16)

    top, bottom = pl.ds(0, HALF), pl.ds(HALF, HALF)

    def ag(k, i, block, rows, to):
        ref = picked.at[k, block] if rows is None else picked.at[k, block, rows]
        return pltpu.make_async_remote_copy(
            src_ref=ref, dst_ref=ref, send_sem=ag_send.at[k, i], recv_sem=ag_recv.at[k, i],
            device_id=to, device_id_type=MESH,
        )

    b_r, b_l, b_f = y_r * 2 + core, y_l * 2 + core, y_f * 2 + core
    t_r, t_l, t_f, t_o = (y_r * 2 + 1 - core, y_l * 2 + 1 - core, y_f * 2 + 1 - core, y * 2 + 1 - core)
    ag_plan = (
        (tp, top, right), (tp, bottom, right), (b_l, top, right),
        (tp, bottom, left), (tp, top, left), (b_r, bottom, left),
        (tp, None, twin),
        (b_l, top, twin), (b_l, bottom, twin), (b_f, top, twin),
        (b_r, bottom, twin), (b_r, top, twin), (b_f, bottom, twin),
    )
    ag_lands = (
        (b_l, top), (b_l, bottom), (b_f, top),
        (b_r, bottom), (b_r, top), (b_f, bottom),
        (t_o, None),
        (t_l, top), (t_l, bottom), (t_f, top),
        (t_r, bottom), (t_r, top), (t_f, bottom),
    )

    def ag_start(k, i):
        block, rows, to = ag_plan[i]
        ag(k, i, block, rows, to).start()

    def ag_arrive(k, i):
        block, rows = ag_lands[i]
        ag(k, i, block, rows, twin).wait_recv()

    def compact(k):
        exchange_wait(arrived, out_recv, k)

        @pl.loop(0, PICKS // STEP)
        def _(i):
            rows = pl.ds(pl.multiple_of(i * STEP, STEP), STEP)
            picked[k, tp, rows, :] = dot(pick[rows, :], arrived[k].reshape(ROWS, LANE)).astype(BF16)

        for i in (0, 3, 1, 4, 6):
            ag_start(k, i)

    def ag_forward(k):
        ag_arrive(k, 0)
        ag_start(k, 2)
        ag_arrive(k, 3)
        ag_start(k, 5)
        ag_start(k, 7)
        ag_start(k, 10)

    def ag_rest(k):
        for i in (1, 4, 2, 5):
            ag_arrive(k, i)
            ag_start(k, i + 7 if i in (1, 2) else i + 7)

    def project(k):
        for i in range(6, 13):
            ag_arrive(k, i)

        @pl.loop(0, PICKS // STEP)
        def _(i):
            rows = pl.ds(pl.multiple_of(i * STEP, STEP), STEP)
            lhs = jnp.concatenate([picked[k, b, rows, :] for b in range(TP)], axis=1)
            for weights, acc in ((gate_w, gate_acc), (up_w, up_acc)):
                rhs = jnp.concatenate(
                    [weights[pl.ds(b * SHARE + k * LANE, LANE), :] for b in range(TP)], axis=0
                )
                part = dot(lhs, rhs)
                if k == 0:
                    acc[rows, :] = part
                elif k < CHUNKS - 1:
                    acc[rows, :] += part
                else:
                    total = acc[rows, :] + part
                    if acc is gate_acc:
                        gate = total
                    else:
                        hidden[rows, :] = (gate / (1.0 + jnp.exp(-gate)) * total).astype(BF16)

    compact(0)
    ag_forward(0)
    compact(1)
    ag_rest(0)
    loads[0].wait()
    loads[1].wait()
    project(0)
    ag_forward(1)
    compact(2)
    ag_rest(1)
    project(1)
    ag_forward(2)
    ag_rest(2)
    project(2)
    loads[2].wait()

    def rs(k, i, src, dst, to):
        return pltpu.make_async_remote_copy(
            src_ref=src, dst_ref=dst, send_sem=rs_send.at[k, i], recv_sem=rs_recv.at[k, i],
            device_id=to, device_id_type=MESH,
        )

    def rs_copy(k, i):
        return (
            lambda: rs(k, 0, twin_out.at[k], twin_in.at[k], twin),
            lambda: rs(k, 1, sums.at[k, y_f, top], ring_l.at[k], right),
            lambda: rs(k, 2, sums.at[k, y_f, bottom], ring_r.at[k], left),
            lambda: rs(k, 3, sums.at[k, y_r, bottom], fin_l.at[k, bottom], right),
            lambda: rs(k, 4, sums.at[k, y_l, top], fin_r.at[k, top], left),
            lambda: rs(k, 5, sums.at[k, y_r, top], fin_l.at[k, top], right),
            lambda: rs(k, 6, sums.at[k, y_l, bottom], fin_r.at[k, bottom], left),
        )[i]()

    def down(k):
        def part(which, target):
            @pl.loop(0, PICKS // STEP)
            def _(i):
                rows = pl.ds(pl.multiple_of(i * STEP, STEP), STEP)
                lhs = hidden[rows, :]
                for pair in range(NY // 2):
                    pieces = []
                    for q in (2 * pair, 2 * pair + 1):
                        start = pl.multiple_of((2 * q + which) * SHARE + k * LANE, LANE)
                        pieces.append(down_w[:, pl.ds(start, LANE)])
                    res = dot(lhs, jnp.concatenate(pieces, axis=1))
                    for n, q in enumerate((2 * pair, 2 * pair + 1)):
                        piece = res[:, n * LANE:(n + 1) * LANE]
                        if target is own_acc:
                            own_acc[q, rows, :] = piece
                        else:
                            target[k, q, rows, :] = piece.astype(BF16)

        part(1 - core, twin_out)
        rs_copy(k, 0).start()
        part(core, own_acc)
        rs_copy(k, 0).wait_recv()

        @pl.loop(0, NY * PICKS // STEP)
        def _(i):
            q = i // (PICKS // STEP)
            rows = pl.ds(pl.multiple_of((i % (PICKS // STEP)) * STEP, STEP), STEP)
            sums[k, q, rows, :] = (own_acc[q, rows, :] + twin_in[k, q, rows, :].astype(F32)).astype(BF16)

        for i in (1, 2, 3, 4):
            rs_copy(k, i).start()

    def rs_forward(k):
        for i, ring, q, rows in ((1, ring_l, y_r, top), (2, ring_r, y_l, bottom)):
            rs_copy(k, i).wait_recv()
            sums[k, q, rows, :] = (
                sums[k, q, rows, :].astype(F32) + ring[k].astype(F32)
            ).astype(BF16)
            rs_copy(k, i + 4).start()

    def give_back(k):
        for i in (3, 4, 5, 6):
            rs_copy(k, i).wait_recv()

        @pl.loop(0, PICKS // STEP)
        def _(i):
            rows = pl.ds(pl.multiple_of(i * STEP, STEP), STEP)
            total = (
                sums[k, y, rows, :].astype(F32) + fin_l[k, rows, :].astype(F32)
                + fin_r[k, rows, :].astype(F32)
            )
            weighted[rows, :] = (total * weight_col[rows, :]).astype(BF16)

        @pl.loop(0, EP // 8)
        def _(i):
            rows = pl.ds(pl.multiple_of(i * 8 * SLOTS, LANE), 8 * SLOTS)
            slab = dot(pick_t[rows, :], weighted[...]).astype(BF16)
            leaving[k, pl.ds(i * 8, 8)] = slab.reshape(8, SLOTS, LANE)

        exchange(leaving, returned, back_send, back_recv, k)
        returned[k, me] = leaving[k, me]

    down(0)
    rs_forward(0)
    down(1)
    give_back(0)
    rs_forward(1)
    down(2)
    give_back(1)
    rs_forward(2)
    give_back(2)

    square = jnp.zeros((TOK, LANE), F32)
    for k in range(CHUNKS):
        exchange_wait(returned, back_recv, k)
        lanes = pl.ds(pl.multiple_of(tp * SHARE + k * LANE, LANE), LANE)
        part = stream[:, lanes].astype(F32) + dot(place_t[...], returned[k].reshape(ROWS, LANE))
        merged[k] = part
        square = square + part * part
    totals[tp] = jnp.broadcast_to(jnp.sum(square.T, axis=0, keepdims=True), (8, TOK))

    def total_copy(j, block):
        return pltpu.make_async_remote_copy(
            src_ref=totals.at[block], dst_ref=totals.at[block],
            send_sem=tot_send.at[j], recv_sem=tot_recv.at[j],
            device_id=(me, (tp + j) % TP), device_id_type=MESH,
        )

    for j in range(1, TP):
        total_copy(j, tp).start()
    for j in range(1, TP):
        total_copy(j, (tp + TP - j) % TP).wait_recv()
    whole = totals[0]
    for b in range(1, TP):
        whole = whole + totals[b]
    for b in range(TOK // LANE):
        rows = slice(b * LANE, (b + 1) * LANE)
        scale = lax.rsqrt(columns_of(whole[0:1, rows]) / WIDTH + EPSILON)
        for k in range(CHUNKS):
            lanes = slice(k * LANE, (k + 1) * LANE)
            out[rows, lanes] = (merged[k, rows, :] * scale * gain_out[:, lanes].astype(F32)).astype(BF16)

    for k in range(CHUNKS):
        exchange_wait(sending, out_send, k)
        exchange_wait(leaving, back_send, k)
        for i in range(13):
            block, rows, to = ag_plan[i]
            ag(k, i, block, rows, to).wait_send()
        for i in range(7):
            rs_copy(k, i).wait_send()
    for j in range(1, TP):
        total_copy(j, tp).wait_send()


def whole_layer(stream, gain_in, gain_out, local_row, arrival_row, affinity_row, gate, up, down):
    vmem = pl.BlockSpec(memory_space=pltpu.VMEM)
    hbm = pl.BlockSpec(memory_space=pl.ANY)
    dma = pltpu.SemaphoreType.DMA
    return pl.pallas_call(
        kernel,
        out_shape=jax.ShapeDtypeStruct((TOK, SHARE), BF16),
        in_specs=[vmem] * 6 + [hbm] * 3,
        out_specs=vmem,
        scratch_shapes=[
            pltpu.VMEM((WIDTH, SHARE), BF16),
            pltpu.VMEM((WIDTH, SHARE), BF16),
            pltpu.VMEM((SHARE, WIDTH), BF16),
            pltpu.VMEM((TOK, SHARE), BF16),
            pltpu.VMEM((ROWS, TOK), BF16),
            pltpu.VMEM((TOK, ROWS), BF16),
            pltpu.VMEM((PICKS, ROWS), BF16),
            pltpu.VMEM((ROWS, PICKS), BF16),
            pltpu.VMEM((PICKS, LANE), F32),
            pltpu.VMEM((CHUNKS, EP, SLOTS, LANE), BF16),
            pltpu.VMEM((CHUNKS, EP, SLOTS, LANE), BF16),
            pltpu.VMEM((CHUNKS, TP, PICKS, LANE), BF16),
            pltpu.VMEM((PICKS, SHARE), F32),
            pltpu.VMEM((PICKS, SHARE), F32),
            pltpu.VMEM((PICKS, SHARE), BF16),
            pltpu.VMEM((NY, PICKS, LANE), F32),
            pltpu.VMEM((CHUNKS, NY, PICKS, LANE), BF16),
            pltpu.VMEM((CHUNKS, NY, PICKS, LANE), BF16),
            pltpu.VMEM((CHUNKS, NY, PICKS, LANE), BF16),
            pltpu.VMEM((CHUNKS, HALF, LANE), BF16),
            pltpu.VMEM((CHUNKS, HALF, LANE), BF16),
            pltpu.VMEM((CHUNKS, PICKS, LANE), BF16),
            pltpu.VMEM((CHUNKS, PICKS, LANE), BF16),
            pltpu.VMEM((PICKS, LANE), BF16),
            pltpu.VMEM((CHUNKS, EP, SLOTS, LANE), BF16),
            pltpu.VMEM((CHUNKS, EP, SLOTS, LANE), BF16),
            pltpu.VMEM((CHUNKS, TOK, LANE), F32),
            pltpu.VMEM((TP, 8, TOK), F32),
            dma((3,)),
            dma((CHUNKS,)),
            dma((CHUNKS,)),
            dma((CHUNKS, 13)),
            dma((CHUNKS, 13)),
            dma((CHUNKS, 7)),
            dma((CHUNKS, 7)),
            dma((CHUNKS,)),
            dma((CHUNKS,)),
            dma((TP,)),
            dma((TP,)),
        ],
        compiler_params=pltpu.CompilerParams(
            collective_id=0, has_side_effects=True, vmem_limit_bytes=60 * 1024 * 1024
        ),
        name="whole_layer",
    )(stream, gain_in, gain_out, local_row, arrival_row, affinity_row, gate, up, down)


def on_device(stream, ffn_gain, chosen, affinity, w_gate, w_up, w_down, final_gain):
    me = lax.axis_index("ep")
    first = jnp.sum((chosen < me * TOK).astype(jnp.int32), axis=1)
    last = jnp.sum((chosen < (me + 1) * TOK).astype(jnp.int32), axis=1)
    slot = jnp.arange(SLOTS, dtype=jnp.int32)
    position = first[:, None] + slot[None, :]
    hit = position[:, :, None] == jnp.arange(PICKS, dtype=jnp.int32)[None, None, :]
    token = jnp.sum(jnp.where(hit, chosen[:, None, :], 0), axis=2) - me * TOK
    local = jnp.where(position < last[:, None], token, -1)
    own = lax.dynamic_index_in_dim(chosen, me, 0, keepdims=False)
    source = own // TOK
    starts = jnp.sum((source[None, :] < jnp.arange(EP, dtype=jnp.int32)[:, None]).astype(jnp.int32), axis=1)
    start = jnp.sum(
        jnp.where(source[None, :] == jnp.arange(EP, dtype=jnp.int32)[:, None], starts[:, None], 0), axis=0
    )
    arrival = source * SLOTS + jnp.arange(PICKS, dtype=jnp.int32) - start
    return whole_layer(
        stream, ffn_gain.reshape(1, -1), final_gain.reshape(1, -1), local.reshape(1, -1),
        arrival.reshape(1, -1), affinity, w_gate[0], w_up[0], w_down[0],
    )


def solution(mesh):
    return jax.shard_map(
        on_device,
        mesh=mesh,
        in_specs=(
            P("ep", None),
            P(),
            P(),
            P("ep", None),
            P("ep", None, "tp"),
            P("ep", None, "tp"),
            P("ep", "tp", None),
            P("tp"),
        ),
        out_specs=P("ep", "tp"),
        check_vma=False,
    )
```
